32 devices in a mesh: sp: 4 (over x, core), dp: 8 (over z, y).
Axes of the slice: x: 2, y: 2, z: 4, core: 2. Of those that a mesh axis runs over, the one named last changes fastest.
Arguments:
- tokens: bfloat16 [8, 1536, 2048], P('dp', 'sp'), may hold values from -6 to 6
- w_value: bfloat16 [2048, 1024], P('dp'), may hold values from -0.125 to 0.125
- w_gate: bfloat16 [2048, 1024], P('dp'), may hold values from -0.125 to 0.125
- conv_taps: bfloat16 [31, 1024], replicated, may hold values from -1 to 1
- norm_gain: bfloat16 [1024], replicated, may hold values from 0.099609375 to 1.8984375
- w_out: bfloat16 [1024, 2048], P(None, 'dp'), may hold values from -0.1875 to 0.1875
Outputs:
- mixed: bfloat16 [8, 1536, 2048], P('dp', 'sp')
The draws below stay inside these ranges and needn't reach their ends.
All inputs are finite; a program needn't handle non-finite values.
Results may differ from the reference program's by a relative error of at most 0.013.
Values may be sent and summed in bfloat16 or wider, within the bound.
No kernel may reach another device: no remote copies, remote signals or barrier semaphores. Data moves between devices by JAX's collectives and lax.ppermute only.
A program may use at most 64 MiB of HBM per device.

```python
import jax
import jax.numpy as jnp
from jax import lax

D = 2048
CONV = 1024
KERNEL = 31
SEQ = 1536
BATCH = 8


def shard_levels(own_key, shape, pieces, low, high):
    gain = 1.0
    for position, blocks in pieces:
        heights = jax.random.uniform(jax.random.fold_in(jax.random.fold_in(own_key, 6), position), (blocks,), jnp.float32, low / len(pieces), high / len(pieces))
        gain = gain * jnp.repeat(jnp.exp(heights), shape[position] // blocks).reshape((-1,) + (1,) * (len(shape) - 1 - position))
    return gain


def normal_values(key, extent, scale, bound, cuts=(), held_as=jnp.bfloat16):
    values = scale * jax.random.normal(key, extent, jnp.float32)
    if cuts:
        values = values * shard_levels(key, extent, cuts, -0.22, 0.18)
    return jnp.clip(values, -bound, bound).astype(held_as)


def setup_inputs(seed: int = 0) -> dict:
    keys = jax.random.split(jax.random.key(seed), 7)
    tokens = normal_values(keys[0], (BATCH, SEQ, D), 1.0, 6.0, ((0, 8), (1, 4)))
    w_value = normal_values(keys[1], (D, CONV), D ** -0.5, 0.125, ((0, 8),))
    w_gate = normal_values(keys[2], (D, CONV), D ** -0.5, 0.125, ((0, 8),))
    conv_taps = normal_values(keys[3], (KERNEL, CONV), KERNEL ** -0.5, 1.0)
    norm_gain = jnp.clip(1.0 + 0.18 * jax.random.normal(keys[4], (CONV,), jnp.float32), 0.099609375, 1.8984375).astype(jnp.bfloat16)
    w_out = normal_values(keys[5], (CONV, D), CONV ** -0.5, 0.1875, ((1, 8),))
    return dict(tokens=tokens, w_value=w_value, w_gate=w_gate, conv_taps=conv_taps, norm_gain=norm_gain, w_out=w_out)


EPSILON = 1e-06

def causal_taps(gated, conv_taps):
    length = gated.shape[0]
    padded = jnp.concatenate([jnp.zeros((KERNEL - 1, CONV), gated.dtype), gated], axis=0).astype(jnp.float32)
    taps_wide = conv_taps.astype(jnp.float32)
    total = jnp.zeros((length, CONV), jnp.float32)
    for shift_pos in range(KERNEL):
        total = total + taps_wide[shift_pos][None, :] * padded[shift_pos:shift_pos + length]
    return total

def per_sequence(sequence, w_value, w_gate, conv_taps, norm_gain, w_out):
    value_part = jnp.dot(sequence, w_value, preferred_element_type=jnp.float32)
    gate_part = jnp.dot(sequence, w_gate, preferred_element_type=jnp.float32)
    gated = (value_part * jax.nn.sigmoid(gate_part)).astype(jnp.bfloat16)
    conv_out = causal_taps(gated, conv_taps).astype(jnp.bfloat16)
    wide = conv_out.astype(jnp.float32)
    chan_mean = lax.optimization_barrier(jnp.mean(wide, -1, keepdims=True))
    centred = wide - chan_mean
    chan_var = lax.optimization_barrier(jnp.mean(centred * centred, -1, keepdims=True))
    normed = centred * lax.rsqrt(chan_var + EPSILON) * norm_gain.astype(jnp.float32)
    activated = (normed * jax.nn.sigmoid(normed)).astype(jnp.bfloat16)
    return jnp.dot(activated, w_out, preferred_element_type=jnp.float32).astype(jnp.bfloat16)

def reference(tokens, w_value, w_gate, conv_taps, norm_gain, w_out):
    return lax.map(lambda sequence: per_sequence(sequence, w_value, w_gate, conv_taps, norm_gain, w_out), tokens)
```

```python
import jax
import jax.numpy as jnp
from jax import lax
from jax.sharding import PartitionSpec as P

EPSILON = 1e-06
DIRECT_LIMIT = 16


def passed_along(x, axis, by):
    length = lax.axis_size(axis)
    pairs = [(i, i + by) for i in range(length) if 0 <= i + by < length]
    return lax.ppermute(x, axis, pairs)


def pair_swap(x):
    return lax.ppermute(x, "dp", [(i, i ^ 1) for i in range(lax.axis_size("dp"))])


def line_shift(x, by):
    size = lax.axis_size("dp")
    return lax.ppermute(x, "dp", [(i, (i + 2 * by) % size) for i in range(size)])


def side_swap(x):
    size = lax.axis_size("sp")
    return lax.ppermute(x, "sp", [(i, (i + size // 2) % size) for i in range(size)])


def core_swap(x):
    return lax.ppermute(x, "sp", [(i, i ^ 1) for i in range(lax.axis_size("sp"))])


def gather_chunks(mine, common, axis):
    slow = lax.axis_size("dp") // 2
    split = mine.shape[axis]
    both = jnp.concatenate([mine, common], axis=axis)
    lines = {by: line_shift(both, by) for by in range(1, slow)}
    pairs = {0: pair_swap(both)}
    for by in range(1, slow):
        pairs[by] = pair_swap(lines[by])
    out = []
    for bit, group in ((0, lines), (1, pairs)):
        for by, full in group.items():
            part = lax.slice_in_dim(full, 0, split, axis=axis)
            out.append((by, bit, full, side_swap(part)))
    return out


def depthwise_conv(signal, local_taps, left_pad):
    kernel_form = jnp.transpose(local_taps)[:, None, :]
    result = lax.conv_general_dilated(
        signal[None],
        kernel_form,
        (1,),
        [(left_pad, 0)],
        dimension_numbers=("NCH", "OIH", "NCH"),
        feature_group_count=signal.shape[0],
        preferred_element_type=jnp.float32,
    )
    return result[0].astype(jnp.bfloat16)


def conv_norm(gated, conv_taps, norm_gain):
    tok_count = gated.shape[0]
    kernel_len = conv_taps.shape[0]
    earlier = passed_along(gated[tok_count - (kernel_len - 1) :], "sp", 1)
    extended = jnp.concatenate([earlier, gated], axis=0)
    conv_out = depthwise_conv(extended.T, conv_taps, 0).T
    wide = conv_out.astype(jnp.float32)
    chan_mean = jnp.mean(wide, 1, keepdims=True)
    centred = wide - chan_mean
    chan_var = jnp.mean(centred * centred, 1, keepdims=True)
    normed = centred * lax.rsqrt(chan_var + EPSILON) * norm_gain.astype(jnp.float32)[None]
    return (normed * jax.nn.sigmoid(normed)).astype(jnp.bfloat16)


def dot32(a, b):
    return jnp.dot(a, b, preferred_element_type=jnp.float32)


def small_body(tokens, w_value, w_gate, conv_taps, norm_gain, w_out):
    seq_rows = tokens[0]
    rows, chans = w_value.shape
    slow = lax.axis_size("dp") // 2
    here = lax.axis_index("dp")
    place = lax.axis_index("sp")
    side = place // (lax.axis_size("sp") // 2)
    first_side = side == 0
    first_core = place % 2 == 0

    def source(by, bit):
        return ((here // 2 - by) % slow) * 2 + (here % 2 + bit) % 2

    def columns(member):
        return lax.dynamic_slice_in_dim(seq_rows, member * rows, rows, axis=1)

    share = 3 * chans // 8
    own_w = jnp.where(first_core, w_value, w_gate)
    mine = jnp.where(first_side, own_w[:, :share], own_w[:, share : 2 * share])
    common = own_w[:, 2 * share :]
    chunks = gather_chunks(mine, common, 1)

    own_cols = columns(here)
    local_value = dot32(own_cols, w_value)
    local_gate = dot32(own_cols, w_gate)

    full_sum, part_sum, full_other, part_other = 0.0, 0.0, 0.0, 0.0
    for by, bit, full, part in chunks:
        cols = columns(source(by, bit))
        full_sum += dot32(cols, full)
        part_sum += dot32(cols, part)
        full_other += dot32(cols, core_swap(full))
        part_other += dot32(cols, core_swap(part))

    def assemble(full, part):
        a = full[:, :share]
        left = jnp.where(first_side, a, part)
        right = jnp.where(first_side, part, a)
        return jnp.concatenate([left, right, full[:, share:]], axis=1)

    own_total = assemble(full_sum, part_sum)
    other_total = assemble(full_other, part_other)
    value_sum = local_value + jnp.where(first_core, own_total, other_total)
    gate_sum = local_gate + jnp.where(first_core, other_total, own_total)
    gated = (value_sum * jax.nn.sigmoid(gate_sum)).astype(jnp.bfloat16)
    activated = conv_norm(gated, conv_taps, norm_gain)

    half = chans // 2
    share_o = 3 * half // 8
    after = chunks[slow - 2][2]
    w_late, _ = lax.optimization_barrier((w_out, after))
    own_o = jnp.where(first_core, w_late[:half], w_late[half:])
    mine_o = jnp.where(first_side, own_o[:share_o], own_o[share_o : 2 * share_o])
    chunks_o = gather_chunks(mine_o, own_o[2 * share_o :], 0)

    def rebuild(full, part):
        a = full[:share_o]
        return jnp.concatenate(
            [jnp.where(first_side, a, part), jnp.where(first_side, part, a), full[share_o:]], axis=0
        )

    width = w_out.shape[1]
    out = jnp.zeros((seq_rows.shape[0], seq_rows.shape[1]), jnp.bfloat16)
    out = lax.dynamic_update_slice_in_dim(
        out, dot32(activated, w_out).astype(jnp.bfloat16), here * width, axis=1
    )
    for by, bit, full, part in chunks_o:
        own = rebuild(full, part)
        other = rebuild(core_swap(full), core_swap(part))
        top = jnp.where(first_core, own, other)
        low = jnp.where(first_core, other, own)
        block = dot32(activated, jnp.concatenate([top, low], axis=0))
        out = lax.dynamic_update_slice_in_dim(
            out, block.astype(jnp.bfloat16), source(by, bit) * width, axis=1
        )
    return out[None]


def large_body(tokens, w_value, w_gate, conv_taps, norm_gain, w_out):
    seq_rows = tokens[0]
    value_sum = dot32(seq_rows, lax.all_gather(w_value, "dp", axis=0, tiled=True))
    gate_sum = dot32(seq_rows, lax.all_gather(w_gate, "dp", axis=0, tiled=True))
    gated = (value_sum * jax.nn.sigmoid(gate_sum)).astype(jnp.bfloat16)
    activated = conv_norm(gated, conv_taps, norm_gain)
    full_out = lax.all_gather(w_out, "dp", axis=1, tiled=True)
    return dot32(activated, full_out).astype(jnp.bfloat16)[None]


def solution(mesh):
    placed = (P("dp", "sp", None), P("dp", None), P("dp", None), P(), P(), P(None, "dp"))
    body = small_body if mesh.shape["dp"] <= DIRECT_LIMIT else large_body
    return jax.shard_map(
        body, mesh=mesh, in_specs=placed, out_specs=P("dp", "sp", None), check_vma=False
    )
```

```python
import jax
import jax.numpy as jnp
from jax import lax
from jax.experimental import pallas as pl
from jax.experimental.pallas import tpu as pltpu
from jax.sharding import PartitionSpec as P

EPSILON = 1e-06
DIRECT_LIMIT = 16


def passed_along(x, axis, by):
    length = lax.axis_size(axis)
    pairs = [(i, i + by) for i in range(length) if 0 <= i + by < length]
    return lax.ppermute(x, axis, pairs)


def pair_swap(x):
    return lax.ppermute(x, "dp", [(i, i ^ 1) for i in range(lax.axis_size("dp"))])


def line_shift(x, by):
    size = lax.axis_size("dp")
    return lax.ppermute(x, "dp", [(i, (i + 2 * by) % size) for i in range(size)])


def side_swap(x):
    size = lax.axis_size("sp")
    return lax.ppermute(x, "sp", [(i, (i + size // 2) % size) for i in range(size)])


def core_swap(x):
    return lax.ppermute(x, "sp", [(i, i ^ 1) for i in range(lax.axis_size("sp"))])


def gather_pieces(mine):
    slow = lax.axis_size("dp") // 2
    lines = {0: mine}
    for by in range(1, slow):
        lines[by] = line_shift(mine, by)
    pairs = {by: pair_swap(piece) for by, piece in lines.items()}
    return [(by, bit, piece) for bit, group in ((0, lines), (1, pairs)) for by, piece in group.items()]


def depthwise_conv(signal, local_taps, left_pad):
    kernel_form = jnp.transpose(local_taps)[:, None, :]
    result = lax.conv_general_dilated(
        signal[None],
        kernel_form,
        (1,),
        [(left_pad, 0)],
        dimension_numbers=("NCH", "OIH", "NCH"),
        feature_group_count=signal.shape[0],
        preferred_element_type=jnp.float32,
    )
    return result[0].astype(jnp.bfloat16)


def conv_norm(gated, conv_taps, norm_gain):
    tok_count = gated.shape[0]
    kernel_len = conv_taps.shape[0]
    earlier = passed_along(gated[tok_count - (kernel_len - 1) :], "sp", 1)
    extended = jnp.concatenate([earlier, gated], axis=0)
    conv_out = depthwise_conv(extended.T, conv_taps, 0).T
    wide = conv_out.astype(jnp.float32)
    chan_mean = jnp.mean(wide, 1, keepdims=True)
    centred = wide - chan_mean
    chan_var = jnp.mean(centred * centred, 1, keepdims=True)
    normed = centred * lax.rsqrt(chan_var + EPSILON) * norm_gain.astype(jnp.float32)[None]
    return (normed * jax.nn.sigmoid(normed)).astype(jnp.bfloat16)


def dot32(a, b):
    return jnp.dot(a, b, preferred_element_type=jnp.float32)


def causal_conv(gated, taps):
    length, chans = gated.shape
    count = taps.shape[0]
    lanes, sublanes = 128, 8
    lead = -(-(count - 1) // sublanes) * sublanes
    skip = lead - (count - 1)
    tile = 128

    def kernel(x_ref, taps_ref, out_ref, wide_ref):
        wide_ref[pl.ds(0, lead), :] = jnp.zeros((lead, chans), jnp.float32)
        wide_ref[pl.ds(lead, length), :] = x_ref[...].astype(jnp.float32)
        for col in range(chans // lanes):
            span = pl.ds(col * lanes, lanes)

            def step(i, carry):
                start = pl.multiple_of(i * tile, tile)
                window = wide_ref[pl.ds(start, tile + lead), span]
                total = jnp.zeros((tile, lanes), jnp.float32)
                for shift in range(sublanes):
                    offsets = [o for o in range(skip, lead + 1) if o % sublanes == shift]
                    if not offsets:
                        continue
                    moved = window[shift : max(offsets) + tile]
                    for o in offsets:
                        at = o - shift
                        weight = taps_ref[pl.ds(o - skip, 1), span]
                        total = total + weight * moved[at : at + tile]
                out_ref[pl.ds(start, tile), span] = total.astype(jnp.bfloat16)
                return carry

            lax.fori_loop(0, length // tile, step, 0)

    return pl.pallas_call(
        kernel,
        out_shape=jax.ShapeDtypeStruct((length, chans), jnp.bfloat16),
        scratch_shapes=[pltpu.VMEM((length + lead, chans), jnp.float32)],
    )(gated, taps)


def dot32(a, b):
    return jnp.dot(a, b, preferred_element_type=jnp.float32)


def small_body(tokens, w_value, w_gate, conv_taps, norm_gain, w_out):
    seq_rows = tokens[0]
    count = seq_rows.shape[0]
    rows, chans = w_value.shape
    dp, sp = lax.axis_size("dp"), lax.axis_size("sp")
    here, place = lax.axis_index("dp"), lax.axis_index("sp")

    def source(by, bit):
        return ((here // 2 - by) % (dp // 2)) * 2 + (here % 2 + bit) % 2

    far_rows = side_swap(seq_rows)
    share = chans // sp
    mine = jnp.concatenate(
        [lax.dynamic_slice_in_dim(w, place * share, share, axis=1) for w in (w_value, w_gate)],
        axis=1,
    )
    pieces = gather_pieces(mine)
    weight = jnp.zeros((rows * dp, 2 * share), mine.dtype)
    for by, bit, piece in pieces:
        weight = lax.dynamic_update_slice_in_dim(weight, piece, source(by, bit) * rows, axis=0)

    half = chans // 2
    w_late, _ = lax.optimization_barrier((w_out, pieces[1][2]))
    core = place % 2
    own_o = lax.dynamic_slice_in_dim(w_late, core * half, half, axis=0)
    width = w_out.shape[1]
    near_o = jnp.zeros((half, width * dp), w_out.dtype)
    for by, bit, piece in gather_pieces(own_o):
        near_o = lax.dynamic_update_slice_in_dim(near_o, piece, source(by, bit) * width, axis=1)
    far_o = core_swap(near_o)

    gated = jnp.zeros((count * sp, share), jnp.bfloat16)
    blocks = (
        (place, seq_rows),
        (place ^ 1, core_swap(seq_rows)),
        ((place + sp // 2) % sp, far_rows),
        ((place ^ 1) + sp // 2, core_swap(far_rows)),
    )
    for index, block in blocks:
        sums = dot32(block, weight)
        part = (sums[:, :share] * jax.nn.sigmoid(sums[:, share:])).astype(jnp.bfloat16)
        gated = lax.dynamic_update_slice_in_dim(gated, part, (index % sp) * count, axis=0)
    own_taps = lax.dynamic_slice_in_dim(conv_taps, place * share, share, axis=1)
    conv_out = causal_conv(gated, own_taps.astype(jnp.float32))

    def rows_of(index):
        return lax.dynamic_slice_in_dim(conv_out, (index % sp) * count, count, axis=0)

    wide = jnp.zeros((count, chans), conv_out.dtype)
    for flip, opposite in ((0, 0), (1, 0), (0, 1), (1, 1)):
        index = (place ^ flip) + opposite * (sp // 2)
        pairs = [(i, ((i ^ flip) + opposite * (sp // 2)) % sp) for i in range(sp)]
        block = rows_of(index)
        if flip or opposite:
            block = lax.ppermute(block, "sp", pairs)
        wide = lax.dynamic_update_slice_in_dim(wide, block, (index % sp) * share, axis=1)

    wide = wide.astype(jnp.float32)
    chan_mean = jnp.mean(wide, 1, keepdims=True)
    centred = wide - chan_mean
    chan_var = jnp.mean(centred * centred, 1, keepdims=True)
    normed = centred * lax.rsqrt(chan_var + EPSILON) * norm_gain.astype(jnp.float32)[None]
    activated = (normed * jax.nn.sigmoid(normed)).astype(jnp.bfloat16)
    near_a = lax.dynamic_slice_in_dim(activated, core * half, half, axis=1)
    far_a = lax.dynamic_slice_in_dim(activated, (1 - core) * half, half, axis=1)
    return (dot32(near_a, near_o) + dot32(far_a, far_o)).astype(jnp.bfloat16)[None]


def large_body(tokens, w_value, w_gate, conv_taps, norm_gain, w_out):
    seq_rows = tokens[0]
    value_sum = dot32(seq_rows, lax.all_gather(w_value, "dp", axis=0, tiled=True))
    gate_sum = dot32(seq_rows, lax.all_gather(w_gate, "dp", axis=0, tiled=True))
    gated = (value_sum * jax.nn.sigmoid(gate_sum)).astype(jnp.bfloat16)
    activated = conv_norm(gated, conv_taps, norm_gain)
    full_out = lax.all_gather(w_out, "dp", axis=1, tiled=True)
    return dot32(activated, full_out).astype(jnp.bfloat16)[None]


def solution(mesh):
    placed = (P("dp", "sp", None), P("dp", None), P("dp", None), P(), P(), P(None, "dp"))
    body = small_body if mesh.shape["dp"] <= DIRECT_LIMIT else large_body
    return jax.shard_map(
        body, mesh=mesh, in_specs=placed, out_specs=P("dp", "sp", None), check_vma=False
    )
```
